1024 devices in a mesh: rep: 2 (over z_hi), fs: 64 (over z_lo, y), tp: 8 (over x, core).
Axes of the slice: x: 4, y: 8, z: 16 (z_hi: 2, z_lo: 8; z = z_hi * 8 + z_lo), core: 2. Of those that a mesh axis runs over, the one named last changes fastest.
Arguments:
- tokens: bfloat16 [65536, 2048], P(('rep', 'fs', 'tp')), may hold values from -6 to 6
- norm_gain: float32 [2048], replicated, may hold values from 0.1 to 1.9
- w_gate: bfloat16 [2048, 3072], P('fs', 'tp'), may hold values from -0.125 to 0.125
- w_up: bfloat16 [2048, 3072], P('fs', 'tp'), may hold values from -0.125 to 0.125
- w_down: bfloat16 [3072, 2048], P('tp', 'fs'), may hold values from -0.109375 to 0.109375
- post_gain: float32 [2048], replicated, may hold values from 0.1 to 1.9
Outputs:
- result: bfloat16 [65536, 2048], P(('rep', 'fs', 'tp'))
The draws below stay inside these ranges and needn't reach their ends.
All inputs are finite; a program needn't handle non-finite values.
Results may differ from the reference program's by a relative error of at most 0.014.
Values may be sent and summed in bfloat16 or wider, within the bound.
No kernel may reach another device: no remote copies, remote signals or barrier semaphores. Data moves between devices by JAX's collectives and lax.ppermute only.
A program may use at most 32 MiB of HBM per device.

```python
import jax
import jax.numpy as jnp
from jax import lax

D = 2048
FF = 3072
TOKENS = 65536
N_TP = 8


def block_scale(own_key, dims, split, smallest, top_value):
    level, own = 1.0, jax.random.fold_in(own_key, 6)
    for axis_at, blocks in split:
        heights = jnp.exp(jax.random.uniform(jax.random.fold_in(own, axis_at), (blocks,), jnp.float32, smallest / len(split), top_value / len(split)))
        level = level * jnp.repeat(heights, dims[axis_at] // blocks).reshape([-1 if axis == axis_at else 1 for axis in range(len(dims))])
    return level


def bell_draw(rng, dims, width, limit, split=(), held_as=jnp.bfloat16):
    values = width * jax.random.normal(rng, dims, jnp.float32)
    if split:
        values = values * block_scale(rng, dims, split, -0.22, 0.18)
    return jnp.clip(values, -limit, limit).astype(held_as)


def setup_inputs(seed: int = 0) -> dict:
    streams_of = jax.random.split(jax.random.key(seed), 7)
    return {
        "tokens": bell_draw(streams_of[0], (TOKENS, D), 1.0, 6.0, ((0, 1024),)),
        "norm_gain": jnp.clip(1.0 + 0.18 * jax.random.normal(streams_of[1], (D,), jnp.float32), 0.1, 1.9),
        "w_gate": bell_draw(streams_of[2], (D, FF), D ** -0.5, 0.125, ((0, 64), (1, 8))),
        "w_up": bell_draw(streams_of[3], (D, FF), D ** -0.5, 0.125, ((0, 64), (1, 8))),
        "w_down": bell_draw(streams_of[4], (FF, D), FF ** -0.5, 0.109375, ((0, 8), (1, 64))),
        "post_gain": jnp.clip(1.0 + 0.18 * jax.random.normal(streams_of[5], (D,), jnp.float32), 0.1, 1.9),
    }


EPS = 1e-06

def rms_scale(values, gain):
    return values * lax.rsqrt(lax.optimization_barrier(jnp.mean(values * values, axis=-1, keepdims=True)) + EPS) * gain

def reference(tokens, norm_gain, w_gate, w_up, w_down, post_gain):
    normed = rms_scale(tokens.astype(jnp.float32), norm_gain).astype(jnp.bfloat16)
    gate = jnp.dot(normed, w_gate, preferred_element_type=jnp.float32)
    up = jnp.dot(normed, w_up, preferred_element_type=jnp.float32)
    hidden = (jax.nn.silu(gate) * up).astype(jnp.bfloat16)
    block = FF // N_TP
    summed = jnp.zeros((tokens.shape[0], D), jnp.float32)
    for index in range(N_TP):
        partial_block = jnp.dot(hidden[:, index * block:(index + 1) * block], w_down[index * block:(index + 1) * block], preferred_element_type=jnp.float32).astype(jnp.bfloat16)
        partial_block = lax.optimization_barrier(partial_block)
        summed = summed + partial_block.astype(jnp.float32)
    return rms_scale(summed, post_gain).astype(jnp.bfloat16)
```

```python
import jax
import jax.numpy as jnp
from jax import lax
from jax.experimental import pallas as pl
from jax.experimental.pallas import tpu as pltpu
from jax.sharding import Mesh
from jax.sharding import PartitionSpec as P

EPS = 1e-06
Z = ("zh", "zl")
ALL = ("zh", "zl", "y", "x", "c")


def rms_scale(values, gain):
    return values * lax.rsqrt(jnp.mean(values * values, axis=-1, keepdims=True) + EPS) * gain


def copy_for_each(x, axis):
    length = lax.axis_size(axis)
    return lax.all_to_all(jnp.broadcast_to(x[None], (length, *x.shape)), axis, 0, 0, tiled=True)


def partner(i, kind, length):
    return (((i + kind) ^ 1) - kind) % length


def exchange(x, axes, length, step):
    pairs = []
    for i in range(length):
        for c in range(2):
            pairs.append((i * 2 + c, partner(i, (c + step) % 2, length) * 2 + c))
    return lax.ppermute(x, (*axes, "c"), pairs)


def slots_of(i, c, length):
    one = lambda v: partner(v, c, length)
    two = lambda v: partner(v, 1 - c, length)
    ids = [i, one(i)]
    ids += [two(i), one(two(i))]
    ids += [two(one(i)), one(two(one(i)))]
    j = two(i)
    ids += [two(one(j)), one(two(one(j)))]
    return [v % 8 for v in ids]


def ff_kernel(ids, normed, *refs):
    a, b = refs[0:5], refs[5:10]
    keep, send, gate_w, up_w, down_w, hid = refs[10:16]
    slot = 0
    for k in range(5):
        for n in range(a[k].shape[0]):
            zi, yi = ids[slot], ids[8 + slot]
            gate_w[zi] = a[k][n, :, 0:32, :]
            down_w[zi, :, 0:16, :] = a[k][n, :, 32:48, :]
            up_w[:, yi] = b[k][n, :, 0:32, :]
            down_w[:, yi, 16:32, :] = b[k][n, :, 32:48, :]
            slot += 1
    x = normed[...].reshape(512, 2048)
    gate = jnp.dot(x, gate_w[...].reshape(2048, 384), preferred_element_type=jnp.float32)
    up = jnp.dot(x, up_w[...].reshape(2048, 384), preferred_element_type=jnp.float32)
    hidden = gate / (1.0 + jnp.exp(-gate)) * up
    hid[...] = hidden.astype(jnp.bfloat16).reshape(4, 2, 64, 384)
    core = ids[16]
    down = down_w[...].reshape(2048, 384)
    nt = (((1,), (1,)), ((), ()))
    for out, which in ((send, 1 - core), (keep, core)):
        rows = hid[:, which].reshape(256, 384)
        part = lax.dot_general(rows, down, nt, preferred_element_type=jnp.float32)
        out[...] = part.astype(jnp.bfloat16).reshape(4, 64, 2048)


def body(tokens, norm_gain, w_gate, w_up, w_down, post_gain):
    w_down_t = w_down.T
    first = jnp.concatenate([w_gate, w_down_t[:16]], axis=0)
    second = jnp.concatenate([w_up, w_down_t[16:]], axis=0)
    a0 = copy_for_each(first, "y")[None]
    b0 = copy_for_each(second, "zl")[None]
    own_normed = rms_scale(tokens.astype(jnp.float32), norm_gain).astype(jnp.bfloat16)
    normed = copy_for_each(own_normed, ("x", "c"))
    a1, b1 = exchange(a0, Z, 16, 0), exchange(b0, ("y",), 8, 0)
    a2 = exchange(jnp.concatenate([a0, a1]), Z, 16, 1)
    b2 = exchange(jnp.concatenate([b0, b1]), ("y",), 8, 1)
    a3, b3 = exchange(a2, Z, 16, 0), exchange(b2, ("y",), 8, 0)
    a4, b4 = exchange(a3, Z, 16, 1), exchange(b3, ("y",), 8, 1)
    core = lax.axis_index("c")
    ids = slots_of(lax.axis_index(Z), core, 16) + slots_of(lax.axis_index("y"), core, 8) + [core]
    ids = jnp.stack([jnp.asarray(v, jnp.int32) for v in ids])
    vmem = pl.BlockSpec(memory_space=pltpu.VMEM)
    part = jax.ShapeDtypeStruct((4, 64, 2048), jnp.bfloat16)
    keep, send = pl.pallas_call(
        ff_kernel,
        out_shape=(part, part),
        in_specs=[pl.BlockSpec(memory_space=pltpu.SMEM)] + [vmem] * 11,
        out_specs=(vmem, vmem),
        scratch_shapes=[
            pltpu.VMEM((8, 8, 32, 384), jnp.bfloat16),
            pltpu.VMEM((8, 8, 32, 384), jnp.bfloat16),
            pltpu.VMEM((8, 8, 32, 384), jnp.bfloat16),
            pltpu.VMEM((4, 2, 64, 384), jnp.bfloat16),
        ],
        compiler_params=pltpu.CompilerParams(vmem_limit_bytes=48 * 1024 * 1024),
        name="ff",
    )(ids, normed, a0, a1, a2, a3, a4, b0, b1, b2, b3, b4)
    other = lax.ppermute(send, "c", [(0, 1), (1, 0)])
    pair = (keep.astype(jnp.float32) + other.astype(jnp.float32)).astype(jnp.bfloat16)
    arrived = lax.all_to_all(pair, "x", split_axis=0, concat_axis=0, tiled=True)
    summed = arrived.astype(jnp.float32).sum(axis=0)
    return rms_scale(summed, post_gain).astype(jnp.bfloat16)


def solution(mesh):
    finer = Mesh(mesh.devices.reshape(2, 8, 8, 4, 2), ALL)
    return jax.shard_map(
        body,
        mesh=finer,
        in_specs=(P(ALL, None), P(), P(("zl", "y"), ("x", "c")), P(("zl", "y"), ("x", "c")), P(("x", "c"), ("zl", "y")), P()),
        out_specs=P(ALL, None),
        check_vma=False,
    )
```

```python
import jax
import jax.numpy as jnp
from jax import lax
from jax.experimental import pallas as pl
from jax.experimental.pallas import tpu as pltpu
from jax.sharding import Mesh
from jax.sharding import PartitionSpec as P

EPS = 1e-06
ALL = ("zh", "zl", "y", "x", "c")
PLANE = ("zh", "zl", "y", "c")


def rms_scale(values, gain):
    return values * lax.rsqrt(jnp.mean(values * values, axis=-1, keepdims=True) + EPS) * gain


def copy_for_each(x, axis, length, groups=None):
    copies = jnp.broadcast_to(x[None], (length, *x.shape))
    return lax.all_to_all(copies, axis, 0, 0, tiled=True, axis_index_groups=groups)


def first_groups():
    at = lambda zh, zl, y, c: ((zh * 8 + zl) * 8 + y) * 2 + c
    groups = [[at(zh, zl, y, 0) for y in range(8)] for zh in range(2) for zl in range(8)]
    return groups + [[at(zh, zl, y, 1) for zl in range(8)] for zh in range(2) for y in range(8)]


def hop(x, by):
    pairs = []
    for z in range(16):
        for y in range(8):
            here = (z * 8 + y) * 2
            pairs.append((here, (((z + by) % 16) * 8 + y) * 2))
            pairs.append((here + 1, (z * 8 + (y + by) % 8) * 2 + 1))
    return lax.ppermute(x, PLANE, pairs)


def ff_kernel(ids, normed, *refs):
    blocks = refs[0:8]
    keep, send, gate_w, up_w, down_w, hid = refs[8:14]
    base, core = ids[0], ids[1]
    weights = (gate_w, up_w, down_w)

    @pl.when(core == 0)
    def _():
        for k, off in enumerate((0, -1, 1, -2, 2, -3, 3, -4)):
            at = (base + (off + 8)) & 7
            for n in range(3):
                weights[n][at] = blocks[k][:, 32 * n : 32 * n + 32, :]

    @pl.when(core == 1)
    def _():
        for k, off in enumerate((0, -1, 1, -2, 2, -3, 3, -4)):
            at = (base + (off + 8)) & 7
            for n in range(3):
                weights[n][:, at] = blocks[k][:, 32 * n : 32 * n + 32, :]

    x = normed[...].reshape(512, 2048)
    gate = jnp.dot(x, gate_w[...].reshape(2048, 384), preferred_element_type=jnp.float32)
    up = jnp.dot(x, up_w[...].reshape(2048, 384), preferred_element_type=jnp.float32)
    hidden = gate / (1.0 + jnp.exp(-gate)) * up
    hid[...] = hidden.astype(jnp.bfloat16).reshape(4, 2, 64, 384)
    down = down_w[...].reshape(2048, 384)
    nt = (((1,), (1,)), ((), ()))
    for out, which in ((send, 1 - core), (keep, core)):
        rows = hid[:, which].reshape(256, 384)
        part = lax.dot_general(rows, down, nt, preferred_element_type=jnp.float32)
        out[...] = part.astype(jnp.bfloat16).reshape(4, 64, 2048)


def body(tokens, norm_gain, w_gate, w_up, w_down, post_gain):
    own = jnp.concatenate([w_gate, w_up, w_down.T], axis=0)
    block = copy_for_each(own, PLANE, 8, first_groups())
    own_normed = rms_scale(tokens.astype(jnp.float32), norm_gain).astype(jnp.bfloat16)
    normed = copy_for_each(own_normed, ("x", "c"), 8)
    blocks = [block]
    up_going = down_going = block
    for k in range(4):
        up_going = hop(up_going, 1)
        blocks.append(up_going)
        if k < 3:
            down_going = hop(down_going, -1)
            blocks.append(down_going)
    core = lax.axis_index("c")
    base = jnp.where(core == 0, lax.axis_index("zl"), lax.axis_index("y"))
    ids = jnp.stack([base, core]).astype(jnp.int32)
    vmem = pl.BlockSpec(memory_space=pltpu.VMEM)
    part = jax.ShapeDtypeStruct((4, 64, 2048), jnp.bfloat16)
    whole = pltpu.VMEM((8, 8, 32, 384), jnp.bfloat16)
    keep, send = pl.pallas_call(
        ff_kernel,
        out_shape=(part, part),
        in_specs=[pl.BlockSpec(memory_space=pltpu.SMEM)] + [vmem] * 9,
        out_specs=(vmem, vmem),
        scratch_shapes=[whole, whole, whole, pltpu.VMEM((4, 2, 64, 384), jnp.bfloat16)],
        compiler_params=pltpu.CompilerParams(vmem_limit_bytes=48 * 1024 * 1024),
        name="ff",
    )(ids, normed, *blocks)
    other = lax.ppermute(send, "c", [(0, 1), (1, 0)])
    pair = (keep.astype(jnp.float32) + other.astype(jnp.float32)).astype(jnp.bfloat16)
    arrived = lax.all_to_all(pair, "x", split_axis=0, concat_axis=0, tiled=True)
    summed = arrived.astype(jnp.float32).sum(axis=0)
    return rms_scale(summed, post_gain).astype(jnp.bfloat16)


def solution(mesh):
    finer = Mesh(mesh.devices.reshape(2, 8, 8, 4, 2), ALL)
    split = P(("zl", "y"), ("x", "c"))
    return jax.shard_map(
        body,
        mesh=finer,
        in_specs=(P(ALL, None), P(), split, split, P(("x", "c"), ("zl", "y")), P()),
        out_specs=P(ALL, None),
        check_vma=False,
    )
```

```python
import jax
import jax.numpy as jnp
from jax import lax
from jax.experimental import pallas as pl
from jax.experimental.pallas import tpu as pltpu
from jax.sharding import Mesh
from jax.sharding import PartitionSpec as P

EPS = 1e-06
ALL = ("zh", "zl", "y", "x", "c")
PLANE = ("zh", "zl", "y", "c")


def rms_scale(values, gain):
    return values * lax.rsqrt(jnp.mean(values * values, axis=-1, keepdims=True) + EPS) * gain


def copy_for_each(x, axis, length, groups=None):
    copies = jnp.broadcast_to(x[None], (length, *x.shape))
    return lax.all_to_all(copies, axis, 0, 0, tiled=True, axis_index_groups=groups)


def first_groups():
    at = lambda zh, zl, y, c: ((zh * 8 + zl) * 8 + y) * 2 + c
    groups = [[at(zh, zl, y, 0) for y in range(8)] for zh in range(2) for zl in range(8)]
    return groups + [[at(zh, zl, y, 1) for zl in range(8)] for zh in range(2) for y in range(8)]


def hop(x, by):
    pairs = []
    for z in range(16):
        for y in range(8):
            here = (z * 8 + y) * 2
            pairs.append((here, (((z + by) % 16) * 8 + y) * 2))
            pairs.append((here + 1, (z * 8 + (y + by) % 8) * 2 + 1))
    return lax.ppermute(x, PLANE, pairs)


def along_x(x, by):
    return lax.ppermute(x, "x", [(i, (i + by) % 4) for i in range(4)])


def ff_kernel(ids, mine, others, *refs):
    blocks = refs[0:8]
    keep, send, gate_w, up_w, down_w = refs[8:13]
    base, core, col = ids[0], ids[1], ids[2]
    weights = (gate_w, up_w, down_w)

    @pl.when(core == 0)
    def _():
        for k, off in enumerate((0, -1, 1, -2, 2, -3, 3, -4)):
            at = (base + (off + 8)) & 7
            for n in range(3):
                weights[n][at] = blocks[k][:, 32 * n : 32 * n + 32, :]

    @pl.when(core == 1)
    def _():
        for k, off in enumerate((0, -1, 1, -2, 2, -3, 3, -4)):
            at = (base + (off + 8)) & 7
            for n in range(3):
                weights[n][:, at] = blocks[k][:, 32 * n : 32 * n + 32, :]

    gates = gate_w[...].reshape(2048, 384)
    ups = up_w[...].reshape(2048, 384)
    down = down_w[...].reshape(2048, 384)
    nt = (((1,), (1,)), ((), ()))
    for rows, out in ((others, send), (mine, keep)):
        x = rows[...].reshape(256, 2048)
        gate = jnp.dot(x, gates, preferred_element_type=jnp.float32)
        up = jnp.dot(x, ups, preferred_element_type=jnp.float32)
        hidden = (gate / (1.0 + jnp.exp(-gate)) * up).astype(jnp.bfloat16)
        part = lax.dot_general(hidden, down, nt, preferred_element_type=jnp.float32)
        part = part.astype(jnp.bfloat16)
        for k, off in enumerate((0, 2, 3, 1)):
            out[(col + off) & 3] = part[64 * k : 64 * k + 64]


def body(tokens, norm_gain, w_gate, w_up, w_down, post_gain):
    own = jnp.concatenate([w_gate, w_up, w_down.T], axis=0)
    block = copy_for_each(own, PLANE, 8, first_groups())
    own_normed = rms_scale(tokens.astype(jnp.float32), norm_gain).astype(jnp.bfloat16)
    near = [along_x(own_normed, by) for by in (2, 1, -1)]
    block, near = lax.optimization_barrier((block, near))
    mine = jnp.stack([own_normed] + near)
    swap = [(0, 1), (1, 0)]
    others = lax.ppermute(mine, "c", swap)
    blocks = [block]
    up_going = down_going = block
    for k in range(4):
        up_going = hop(up_going, 1)
        blocks.append(up_going)
        if k < 3:
            down_going = hop(down_going, -1)
            blocks.append(down_going)
    core = lax.axis_index("c")
    base = jnp.where(core == 0, lax.axis_index("zl"), lax.axis_index("y"))
    ids = jnp.stack([base, core, lax.axis_index("x")]).astype(jnp.int32)
    vmem = pl.BlockSpec(memory_space=pltpu.VMEM)
    part = jax.ShapeDtypeStruct((4, 64, 2048), jnp.bfloat16)
    whole = pltpu.VMEM((8, 8, 32, 384), jnp.bfloat16)
    keep, send = pl.pallas_call(
        ff_kernel,
        out_shape=(part, part),
        in_specs=[pl.BlockSpec(memory_space=pltpu.SMEM)] + [vmem] * 10,
        out_specs=(vmem, vmem),
        scratch_shapes=[whole, whole, whole],
        compiler_params=pltpu.CompilerParams(vmem_limit_bytes=48 * 1024 * 1024),
        name="ff",
    )(ids, mine, others, *blocks)
    other = lax.ppermute(send, "c", swap)
    pair = (keep.astype(jnp.float32) + other.astype(jnp.float32)).astype(jnp.bfloat16)
    arrived = lax.all_to_all(pair, "x", split_axis=0, concat_axis=0, tiled=True)
    summed = arrived.astype(jnp.float32).sum(axis=0)
    return rms_scale(summed, post_gain).astype(jnp.bfloat16)


def solution(mesh):
    finer = Mesh(mesh.devices.reshape(2, 8, 8, 4, 2), ALL)
    split = P(("zl", "y"), ("x", "c"))
    return jax.shard_map(
        body,
        mesh=finer,
        in_specs=(P(ALL, None), P(), split, split, P(("x", "c"), ("zl", "y")), P()),
        out_specs=P(ALL, None),
        check_vma=False,
    )
```

```python
import jax
import jax.numpy as jnp
from jax import lax
from jax.experimental import pallas as pl
from jax.experimental.pallas import tpu as pltpu
from jax.sharding import Mesh
from jax.sharding import PartitionSpec as P

EPS = 1e-06
ALL = ("zh", "zl", "y", "x", "c")
PLANE = ("zh", "zl", "y")


def rms_scale(values, gain):
    return values * lax.rsqrt(jnp.mean(values * values, axis=-1, keepdims=True) + EPS) * gain


def copy_for_each(x, axis):
    copies = jnp.broadcast_to(x[None], (lax.axis_size(axis), *x.shape))
    return lax.all_to_all(copies, axis, 0, 0, tiled=True)


def own_half(w):
    return lax.dynamic_slice_in_dim(w, lax.axis_index("zh") * 16, 16, axis=0)


def ff_kernel(ids, normed, rows, keep, send, gate_w, up_w, down_w, hid):
    core = ids[0]
    for half in range(2):
        part = slice(16 * half, 16 * half + 16)
        gate_w[:, part] = rows[half, :, 0:16]
        up_w[:, part] = rows[half, :, 16:32]
        down_w[:, part] = rows[half, :, 32:48]
    x = normed[...].reshape(512, 2048)
    gate = jnp.dot(x, gate_w[...].reshape(2048, 384), preferred_element_type=jnp.float32)
    up = jnp.dot(x, up_w[...].reshape(2048, 384), preferred_element_type=jnp.float32)
    hidden = gate / (1.0 + jnp.exp(-gate)) * up
    hid[...] = hidden.astype(jnp.bfloat16).reshape(4, 2, 64, 384)
    down = down_w[...].reshape(2048, 384)
    nt = (((1,), (1,)), ((), ()))
    for out, which in ((send, 1 - core), (keep, core)):
        rows = hid[:, which].reshape(256, 384)
        part = lax.dot_general(rows, down, nt, preferred_element_type=jnp.float32)
        out[...] = part.astype(jnp.bfloat16).reshape(4, 64, 2048)


def body(tokens, norm_gain, w_gate, w_up, w_down, post_gain):
    halves = [own_half(w) for w in (w_gate, w_up, w_down.T)]
    rows = lax.all_gather(jnp.concatenate(halves, axis=0), PLANE, axis=0)
    rows = rows.reshape(2, 64, 48, 384)
    own_normed = rms_scale(tokens.astype(jnp.float32), norm_gain).astype(jnp.bfloat16)
    normed = copy_for_each(own_normed, ("x", "c"))
    ids = lax.axis_index("c").astype(jnp.int32)[None]
    vmem = pl.BlockSpec(memory_space=pltpu.VMEM)
    part = jax.ShapeDtypeStruct((4, 64, 2048), jnp.bfloat16)
    whole = pltpu.VMEM((64, 32, 384), jnp.bfloat16)
    keep, send = pl.pallas_call(
        ff_kernel,
        out_shape=(part, part),
        in_specs=[pl.BlockSpec(memory_space=pltpu.SMEM)] + [vmem] * 2,
        out_specs=(vmem, vmem),
        scratch_shapes=[whole, whole, whole, pltpu.VMEM((4, 2, 64, 384), jnp.bfloat16)],
        compiler_params=pltpu.CompilerParams(vmem_limit_bytes=48 * 1024 * 1024),
        name="ff",
    )(ids, normed, rows)
    other = lax.ppermute(send, "c", [(0, 1), (1, 0)])
    pair = (keep.astype(jnp.float32) + other.astype(jnp.float32)).astype(jnp.bfloat16)
    arrived = lax.all_to_all(pair, "x", split_axis=0, concat_axis=0, tiled=True)
    summed = arrived.astype(jnp.float32).sum(axis=0)
    return rms_scale(summed, post_gain).astype(jnp.bfloat16)


def solution(mesh):
    finer = Mesh(mesh.devices.reshape(2, 8, 8, 4, 2), ALL)
    split = P(("zl", "y"), ("x", "c"))
    return jax.shard_map(
        body,
        mesh=finer,
        in_specs=(P(ALL, None), P(), split, split, P(("x", "c"), ("zl", "y")), P()),
        out_specs=P(ALL, None),
        check_vma=False,
    )
```

```python
import jax
import jax.numpy as jnp
from jax import lax
from jax.experimental import pallas as pl
from jax.experimental.pallas import tpu as pltpu
from jax.sharding import Mesh
from jax.sharding import PartitionSpec as P

EPS = 1e-06
ALL = ("zh", "zl", "y", "x", "c")
PLANE = ("zh", "zl", "y", "c")


def rms_scale(values, gain):
    return values * lax.rsqrt(jnp.mean(values * values, axis=-1, keepdims=True) + EPS) * gain


def copy_for_each(x, axis, length, groups=None):
    copies = jnp.broadcast_to(x[None], (length, *x.shape))
    return lax.all_to_all(copies, axis, 0, 0, tiled=True, axis_index_groups=groups)


def at(z, y, c):
    return ((z % 16) * 8 + y % 8) * 2 + c


def first_groups():
    groups = []
    for c in range(2):
        for r in range(4):
            for z in (r, r + 8):
                z += 4 * ((r + c) % 2)
                for odd in range(2):
                    groups.append([at(z + 4 * ((y + odd) % 2), y, c) for y in range(8)])
    return groups


def partner(i, kind):
    return ((i + kind) ^ 1) - kind


def exchange_z(x, kind):
    pairs = []
    for z in range(16):
        for y in range(8):
            for c in range(2):
                pairs.append((at(z, y, c), at(partner(z, kind), y, c)))
    return lax.ppermute(x, PLANE, pairs)


def exchange_y(x):
    pairs = []
    for z in range(16):
        for y in range(8):
            for c in range(2):
                pairs.append((at(z, y, c), at(z, partner(y, c), c)))
    return lax.ppermute(x, PLANE, pairs)


def ff_kernel(ids, normed, *refs):
    blocks = refs[0:8]
    keep, send, gate_w, up_w, down_w, hid = refs[8:14]
    own, step, core = ids[0], ids[1], ids[2]
    classes = [own + d for d in (0, step, -step, 2 * step, -2 * step, 4, 4 + step, 4 - step)]
    for blk, k in zip(blocks, classes):
        for n, w in enumerate((gate_w, up_w, down_w)):
            for odd in range(2):
                w[(k + 8 + 4 * odd) & 7, :, odd] = blk[:, odd, 32 * n : 32 * n + 32]
    x = normed[...].reshape(512, 2048)
    gate = jnp.dot(x, gate_w[...].reshape(2048, 384), preferred_element_type=jnp.float32)
    up = jnp.dot(x, up_w[...].reshape(2048, 384), preferred_element_type=jnp.float32)
    hidden = gate / (1.0 + jnp.exp(-gate)) * up
    hid[...] = hidden.astype(jnp.bfloat16).reshape(4, 2, 64, 384)
    down = down_w[...].reshape(2048, 384)
    nt = (((1,), (1,)), ((), ()))
    for out, which in ((send, 1 - core), (keep, core)):
        rows = hid[:, which].reshape(256, 384)
        part = lax.dot_general(rows, down, nt, preferred_element_type=jnp.float32)
        out[...] = part.astype(jnp.bfloat16).reshape(4, 64, 2048)


def body(tokens, norm_gain, w_gate, w_up, w_down, post_gain):
    own = jnp.concatenate([w_gate, w_up, w_down.T], axis=0)
    block = copy_for_each(own, PLANE, 8, first_groups())
    own_normed = rms_scale(tokens.astype(jnp.float32), norm_gain).astype(jnp.bfloat16)
    normed = copy_for_each(own_normed, ("x", "c"), 8)
    even, odd, across = exchange_z(block, 0), exchange_z(block, 1), exchange_y(block)
    far_odd, across_even = exchange_z(even, 1), exchange_y(even)
    far_even, across_odd = exchange_z(odd, 0), exchange_y(odd)
    blocks = [block, even, odd, far_even, far_odd, across, across_even, across_odd]
    blocks = [b.reshape(4, 2, 96, 384) for b in blocks]
    z, y, core = lax.axis_index("zl"), lax.axis_index("y"), lax.axis_index("c")
    ids = jnp.stack([z + 4 * (y & 1), 1 - 2 * (z & 1), core]).astype(jnp.int32)
    vmem = pl.BlockSpec(memory_space=pltpu.VMEM)
    part = jax.ShapeDtypeStruct((4, 64, 2048), jnp.bfloat16)
    whole = pltpu.VMEM((8, 4, 2, 32, 384), jnp.bfloat16)
    keep, send = pl.pallas_call(
        ff_kernel,
        out_shape=(part, part),
        in_specs=[pl.BlockSpec(memory_space=pltpu.SMEM)] + [vmem] * 9,
        out_specs=(vmem, vmem),
        scratch_shapes=[whole, whole, whole, pltpu.VMEM((4, 2, 64, 384), jnp.bfloat16)],
        compiler_params=pltpu.CompilerParams(vmem_limit_bytes=48 * 1024 * 1024),
        name="ff",
    )(ids, normed, *blocks)
    other = lax.ppermute(send, "c", [(0, 1), (1, 0)])
    pair = (keep.astype(jnp.float32) + other.astype(jnp.float32)).astype(jnp.bfloat16)
    arrived = lax.all_to_all(pair, "x", split_axis=0, concat_axis=0, tiled=True)
    summed = arrived.astype(jnp.float32).sum(axis=0)
    return rms_scale(summed, post_gain).astype(jnp.bfloat16)


def solution(mesh):
    finer = Mesh(mesh.devices.reshape(2, 8, 8, 4, 2), ALL)
    split = P(("zl", "y"), ("x", "c"))
    return jax.shard_map(
        body,
        mesh=finer,
        in_specs=(P(ALL, None), P(), split, split, P(("x", "c"), ("zl", "y")), P()),
        out_specs=P(ALL, None),
        check_vma=False,
    )
```

```python
import jax
import jax.numpy as jnp
from jax import lax
from jax.experimental import pallas as pl
from jax.experimental.pallas import tpu as pltpu
from jax.sharding import Mesh
from jax.sharding import PartitionSpec as P


EPS = 1e-06
ALL = ("zh", "zl", "y", "x", "c")
PLANE = ("zh", "zl", "y", "c")


def rms_scale(values, gain):
    return values * lax.rsqrt(jnp.mean(values * values, axis=-1, keepdims=True) + EPS) * gain


def copy_for_each(x, axis, length, groups=None):
    copies = jnp.broadcast_to(x[None], (length, *x.shape))
    return lax.all_to_all(copies, axis, 0, 0, tiled=True, axis_index_groups=groups)


def first_groups():
    at = lambda zh, zl, y, c: ((zh * 8 + zl) * 8 + y) * 2 + c
    groups = [[at(zh, zl, y, 0) for y in range(8)] for zh in range(2) for zl in range(8)]
    return groups + [[at(zh, zl, y, 1) for zl in range(8)] for zh in range(2) for y in range(8)]


def partner(i, kind):
    return ((i + kind) ^ 1) - kind


def exchange(x, kind):
    pairs = []
    for z in range(16):
        for y in range(8):
            here = (z * 8 + y) * 2
            pairs.append((here, (partner(z, kind) % 16 * 8 + y) * 2))
            pairs.append((here + 1, (z * 8 + partner(y, kind) % 8) * 2 + 1))
    return lax.ppermute(x, PLANE, pairs)


def ff_kernel(ids, normed, *refs):
    blocks = refs[0:8]
    keep, send, gate_w, up_w, down_w, hid = refs[8:14]
    base, core = ids[0], ids[1]
    side = 1 - 2 * (base & 1)
    weights = (gate_w, up_w, down_w)
    classes = [(base + 8 + n * side) & 7 for n in (0, 1, -1, 2, -2, 3, -3, 4)]

    @pl.when(core == 0)
    def _():
        for blk, at in zip(blocks, classes):
            for n in range(3):
                weights[n][at] = blk[:, 32 * n : 32 * n + 32, :]

    @pl.when(core == 1)
    def _():
        for blk, at in zip(blocks, classes):
            for n in range(3):
                weights[n][:, at] = blk[:, 32 * n : 32 * n + 32, :]

    x = normed[...].reshape(512, 2048)
    gate = jnp.dot(x, gate_w[...].reshape(2048, 384), preferred_element_type=jnp.float32)
    up = jnp.dot(x, up_w[...].reshape(2048, 384), preferred_element_type=jnp.float32)
    hidden = gate / (1.0 + jnp.exp(-gate)) * up
    hid[...] = hidden.astype(jnp.bfloat16).reshape(4, 2, 64, 384)
    down = down_w[...].reshape(2048, 384)
    nt = (((1,), (1,)), ((), ()))
    for out, which in ((send, 1 - core), (keep, core)):
        rows = hid[:, which].reshape(256, 384)
        part = lax.dot_general(rows, down, nt, preferred_element_type=jnp.float32)
        out[...] = part.astype(jnp.bfloat16).reshape(4, 64, 2048)


def body(tokens, norm_gain, w_gate, w_up, w_down, post_gain):
    own = jnp.concatenate([w_gate, w_up, w_down.T], axis=0)
    block = copy_for_each(own, PLANE, 8, first_groups())
    own_normed = rms_scale(tokens.astype(jnp.float32), norm_gain).astype(jnp.bfloat16)
    copies = jnp.broadcast_to(own_normed[None], (8, *own_normed.shape))
    block, copies = lax.optimization_barrier((block, copies))
    blocks = [block]
    even = odd = block
    for k in range(4):
        new_even = exchange(odd, 0)
        blocks.append(new_even)
        if k < 3:
            odd = exchange(even, 1)
            blocks.append(odd)
        even = new_even
    normed = lax.all_to_all(copies, ("x", "c"), 0, 0, tiled=True)
    core = lax.axis_index("c")
    base = jnp.where(core == 0, lax.axis_index("zl"), lax.axis_index("y"))
    ids = jnp.stack([base, core]).astype(jnp.int32)
    vmem = pl.BlockSpec(memory_space=pltpu.VMEM)
    part = jax.ShapeDtypeStruct((4, 64, 2048), jnp.bfloat16)
    whole = pltpu.VMEM((8, 8, 32, 384), jnp.bfloat16)
    keep, send = pl.pallas_call(
        ff_kernel,
        out_shape=(part, part),
        in_specs=[pl.BlockSpec(memory_space=pltpu.SMEM)] + [vmem] * 9,
        out_specs=(vmem, vmem),
        scratch_shapes=[whole, whole, whole, pltpu.VMEM((4, 2, 64, 384), jnp.bfloat16)],
        compiler_params=pltpu.CompilerParams(vmem_limit_bytes=48 * 1024 * 1024),
        name="ff",
    )(ids, normed, *blocks)
    other = lax.ppermute(send, "c", [(0, 1), (1, 0)])
    pair = (keep.astype(jnp.float32) + other.astype(jnp.float32)).astype(jnp.bfloat16)
    arrived = lax.all_to_all(pair, "x", split_axis=0, concat_axis=0, tiled=True)
    summed = arrived.astype(jnp.float32).sum(axis=0)
    return rms_scale(summed, post_gain).astype(jnp.bfloat16)


def solution(mesh):
    finer = Mesh(mesh.devices.reshape(2, 8, 8, 4, 2), ALL)
    split = P(("zl", "y"), ("x", "c"))
    return jax.shard_map(
        body,
        mesh=finer,
        in_specs=(P(ALL, None), P(), split, split, P(("x", "c"), ("zl", "y")), P()),
        out_specs=P(ALL, None),
        check_vma=False,
    )
```

```python
import jax
import jax.numpy as jnp
from jax import lax
from jax.experimental import pallas as pl
from jax.experimental.pallas import tpu as pltpu
from jax.sharding import Mesh
from jax.sharding import PartitionSpec as P


EPS = 1e-06
ALL = ("zh", "zl", "y", "x", "c")
PLANE = ("zh", "zl", "y", "c")


def rms_scale(values, gain):
    return values * lax.rsqrt(jnp.mean(values * values, axis=-1, keepdims=True) + EPS) * gain


def first_groups():
    at = lambda zh, zl, y, c: ((zh * 8 + zl) * 8 + y) * 2 + c
    groups = [[at(zh, zl, y, 0) for y in range(8)] for zh in range(2) for zl in range(8)]
    return groups + [[at(zh, zl, y, 1) for zl in range(8)] for zh in range(2) for y in range(8)]


def partner(i, kind):
    return ((i + kind) ^ 1) - kind


def exchange(x, kind):
    pairs = []
    for z in range(16):
        for y in range(8):
            here = (z * 8 + y) * 2
            pairs.append((here, (partner(z, kind) % 16 * 8 + y) * 2))
            pairs.append((here + 1, (z * 8 + partner(y, kind) % 8) * 2 + 1))
    return lax.ppermute(x, PLANE, pairs)


def most_kernel(ids, normed, *refs):
    blocks = refs[0:7]
    gate_up, x_last, down, gate_w, up_w = refs[7:12]
    base, core = ids[0], ids[1]
    side = 1 - 2 * (base & 1)
    weights = (gate_w, up_w, down)
    classes = [(base + 8 + n * side) & 7 for n in (0, 1, -1, 2, -2, 3, -3)]
    last = (base + 4) & 7
    empty = jnp.zeros((8, 32, 384), jnp.bfloat16)

    @pl.when(core == 0)
    def _():
        for n, w in enumerate(weights):
            w[last] = empty
            for blk, at in zip(blocks, classes):
                w[at] = blk[:, 32 * n : 32 * n + 32, :]

    @pl.when(core == 1)
    def _():
        for n, w in enumerate(weights):
            w[:, last] = empty
            for blk, at in zip(blocks, classes):
                w[:, at] = blk[:, 32 * n : 32 * n + 32, :]

    x = normed[...].reshape(512, 2048)
    for n, w in enumerate((gate_w, up_w)):
        acc = jnp.dot(x, w[...].reshape(2048, 384), preferred_element_type=jnp.float32)
        gate_up[n] = acc.reshape(4, 2, 64, 384)
    row = lax.broadcasted_iota(jnp.int32, (2048, 256), 0)
    j = lax.broadcasted_iota(jnp.int32, (2048, 256), 1)
    wanted = jnp.where(core == 0, last * 256 + j, (j >> 5) * 256 + last * 32 + (j & 31))
    pick = jnp.where(row == wanted, 1.0, 0.0).astype(jnp.bfloat16)
    picked = jnp.dot(x, pick, preferred_element_type=jnp.float32)
    x_last[...] = picked.astype(jnp.bfloat16).reshape(4, 2, 64, 256)


def last_kernel(ids, gate_up, x_last, most_down, half_0, half_1, out, down):
    base, core, which = ids[0], ids[1], ids[2]
    last = (base + 4) & 7
    halves = (half_0, half_1)
    down[...] = most_down[...]

    @pl.when(core == 0)
    def _():
        for h, half in enumerate(halves):
            down[last, 4 * h : 4 * h + 4] = half[:, 64:96, :]

    @pl.when(core == 1)
    def _():
        for h, half in enumerate(halves):
            down[4 * h : 4 * h + 4, last] = half[:, 64:96, :]

    x = x_last[:, which].reshape(256, 256)
    sums = []
    for n in range(2):
        acc = gate_up[n, :, which].reshape(256, 384)
        for h, half in enumerate(halves):
            w = half[:, 32 * n : 32 * n + 32, :].reshape(128, 384)
            acc = acc + jnp.dot(x[:, 128 * h : 128 * h + 128], w, preferred_element_type=jnp.float32)
        sums.append(acc)
    gate, up = sums
    hidden = (gate / (1.0 + jnp.exp(-gate)) * up).astype(jnp.bfloat16)
    nt = (((1,), (1,)), ((), ()))
    part = lax.dot_general(hidden, down[...].reshape(2048, 384), nt, preferred_element_type=jnp.float32)
    out[...] = part.astype(jnp.bfloat16).reshape(4, 64, 2048)


VMEM = pl.BlockSpec(memory_space=pltpu.VMEM)
SMEM = pl.BlockSpec(memory_space=pltpu.SMEM)
WHOLE = (8, 8, 32, 384)


def most_of(ids, normed, blocks):
    return pl.pallas_call(
        most_kernel,
        out_shape=(
            jax.ShapeDtypeStruct((2, 4, 2, 64, 384), jnp.float32),
            jax.ShapeDtypeStruct((4, 2, 64, 256), jnp.bfloat16),
            jax.ShapeDtypeStruct(WHOLE, jnp.bfloat16),
        ),
        in_specs=[SMEM] + [VMEM] * 8,
        out_specs=(VMEM, VMEM, VMEM),
        scratch_shapes=[pltpu.VMEM(WHOLE, jnp.bfloat16)] * 2,
        compiler_params=pltpu.CompilerParams(vmem_limit_bytes=50 * 1024 * 1024),
        name="most",
    )(ids, normed, *blocks)


def partial_of(ids, most, halves):
    return pl.pallas_call(
        last_kernel,
        out_shape=jax.ShapeDtypeStruct((4, 64, 2048), jnp.bfloat16),
        in_specs=[SMEM] + [VMEM] * 5,
        out_specs=VMEM,
        scratch_shapes=[pltpu.VMEM(WHOLE, jnp.bfloat16)],
        compiler_params=pltpu.CompilerParams(vmem_limit_bytes=16 * 1024 * 1024),
    )(ids, *most, *halves)


def body(tokens, norm_gain, w_gate, w_up, w_down, post_gain):
    own = jnp.concatenate([w_gate, w_up, w_down.T], axis=0)
    own = jnp.broadcast_to(own[None], (8, *own.shape))
    block = lax.all_to_all(own, PLANE, 0, 0, tiled=True, axis_index_groups=first_groups())
    own_normed = rms_scale(tokens.astype(jnp.float32), norm_gain).astype(jnp.bfloat16)
    copies = jnp.broadcast_to(own_normed[None], (8, *own_normed.shape))
    block, copies = lax.optimization_barrier((block, copies))
    blocks = [block]
    even = odd = block
    for _ in range(3):
        new_even = exchange(odd, 0)
        odd = exchange(even, 1)
        even = new_even
        blocks += [even, odd]
    half_0 = exchange(odd[:4], 0)
    half_1 = exchange(even[4:], 1)
    normed = lax.all_to_all(copies, ("x", "c"), 0, 0, tiled=True)
    core = lax.axis_index("c")
    base = jnp.where(core == 0, lax.axis_index("zl"), lax.axis_index("y"))
    ids = jnp.stack([base, core, 1 - core]).astype(jnp.int32)
    most = most_of(ids, normed, blocks)
    send = partial_of(ids, most, (half_0, half_1))
    other = lax.ppermute(send, "c", [(0, 1), (1, 0)])
    ids = jnp.stack([base, core, core]).astype(jnp.int32)
    keep = partial_of(ids, most, (half_0, half_1))
    pair = (keep.astype(jnp.float32) + other.astype(jnp.float32)).astype(jnp.bfloat16)
    arrived = lax.all_to_all(pair, "x", split_axis=0, concat_axis=0, tiled=True)
    summed = arrived.astype(jnp.float32).sum(axis=0)
    return rms_scale(summed, post_gain).astype(jnp.bfloat16)


def solution(mesh):
    finer = Mesh(mesh.devices.reshape(2, 8, 8, 4, 2), ALL)
    split = P(("zl", "y"), ("x", "c"))
    return jax.shard_map(
        body,
        mesh=finer,
        in_specs=(P(ALL, None), P(), split, split, P(("x", "c"), ("zl", "y")), P()),
        out_specs=P(ALL, None),
        check_vma=False,
    )
```

```python
import jax
import jax.numpy as jnp
from jax import lax
from jax.experimental import pallas as pl
from jax.experimental.pallas import tpu as pltpu
from jax.sharding import Mesh
from jax.sharding import PartitionSpec as P


EPS = 1e-06
ALL = ("zh", "zl", "y", "x", "c")
PLANE = ("zh", "zl", "y", "c")


def rms_scale(values, gain):
    return values * lax.rsqrt(jnp.mean(values * values, axis=-1, keepdims=True) + EPS) * gain


def first_groups():
    at = lambda zh, zl, y, c: ((zh * 8 + zl) * 8 + y) * 2 + c
    groups = [[at(zh, zl, y, 0) for y in range(8)] for zh in range(2) for zl in range(8)]
    return groups + [[at(zh, zl, y, 1) for zl in range(8)] for zh in range(2) for y in range(8)]


def partner(i, kind):
    return ((i + kind) ^ 1) - kind


def exchange(x, kind):
    pairs = []
    for z in range(16):
        for y in range(8):
            here = (z * 8 + y) * 2
            pairs.append((here, (partner(z, kind) % 16 * 8 + y) * 2))
            pairs.append((here + 1, (z * 8 + partner(y, kind) % 8) * 2 + 1))
    return lax.ppermute(x, PLANE, pairs)


def most_kernel(ids, normed, *refs):
    blocks = refs[0:7]
    gate_up, x_last, down, gate_w, up_w = refs[7:12]
    base, core = ids[0], ids[1]
    side = 1 - 2 * (base & 1)
    weights = (gate_w, up_w, down)
    classes = [(base + 8 + n * side) & 7 for n in (0, 1, -1, 2, -2, 3, -3)]
    last = (base + 4) & 7
    empty = jnp.zeros((8, 32, 384), jnp.bfloat16)

    @pl.when(core == 0)
    def _():
        for n, w in enumerate(weights):
            w[last] = empty
            for blk, at in zip(blocks, classes):
                w[at] = blk[:, 32 * n : 32 * n + 32, :]

    @pl.when(core == 1)
    def _():
        for n, w in enumerate(weights):
            w[:, last] = empty
            for blk, at in zip(blocks, classes):
                w[:, at] = blk[:, 32 * n : 32 * n + 32, :]

    x = normed[...].reshape(512, 2048)
    for n, w in enumerate((gate_w, up_w)):
        acc = jnp.dot(x, w[...].reshape(2048, 384), preferred_element_type=jnp.float32)
        gate_up[n] = acc.reshape(4, 2, 64, 384)
    row = lax.broadcasted_iota(jnp.int32, (2048, 256), 0)
    j = lax.broadcasted_iota(jnp.int32, (2048, 256), 1)
    wanted = jnp.where(core == 0, last * 256 + j, (j >> 5) * 256 + last * 32 + (j & 31))
    pick = jnp.where(row == wanted, 1.0, 0.0).astype(jnp.bfloat16)
    picked = jnp.dot(x, pick, preferred_element_type=jnp.float32)
    x_last[...] = picked.astype(jnp.bfloat16).reshape(4, 2, 64, 256)


def last_kernel(ids, gate_up, x_last, most_down, blk, out, down):
    base, core, which = ids[0], ids[1], ids[2]
    last = (base + 4) & 7
    down[...] = most_down[...]

    @pl.when(core == 0)
    def _():
        down[last] = blk[:, 64:96, :]

    @pl.when(core == 1)
    def _():
        down[:, last] = blk[:, 64:96, :]

    x = x_last[:, which].reshape(256, 256)
    sums = []
    for n in range(2):
        w = blk[:, 32 * n : 32 * n + 32, :].reshape(256, 384)
        rest = jnp.dot(x, w, preferred_element_type=jnp.float32)
        sums.append(gate_up[n, :, which].reshape(256, 384) + rest)
    gate, up = sums
    hidden = (gate / (1.0 + jnp.exp(-gate)) * up).astype(jnp.bfloat16)
    nt = (((1,), (1,)), ((), ()))
    part = lax.dot_general(hidden, down[...].reshape(2048, 384), nt, preferred_element_type=jnp.float32)
    out[...] = part.astype(jnp.bfloat16).reshape(4, 64, 2048)


VMEM = pl.BlockSpec(memory_space=pltpu.VMEM)
SMEM = pl.BlockSpec(memory_space=pltpu.SMEM)
WHOLE = (8, 8, 32, 384)


def most_of(ids, normed, blocks):
    return pl.pallas_call(
        most_kernel,
        out_shape=(
            jax.ShapeDtypeStruct((2, 4, 2, 64, 384), jnp.float32),
            jax.ShapeDtypeStruct((4, 2, 64, 256), jnp.bfloat16),
            jax.ShapeDtypeStruct(WHOLE, jnp.bfloat16),
        ),
        in_specs=[SMEM] + [VMEM] * 8,
        out_specs=(VMEM, VMEM, VMEM),
        scratch_shapes=[pltpu.VMEM(WHOLE, jnp.bfloat16)] * 2,
        compiler_params=pltpu.CompilerParams(vmem_limit_bytes=46 * 1024 * 1024),
        name="most",
    )(ids, normed, *blocks)


def partial_of(ids, most, block):
    return pl.pallas_call(
        last_kernel,
        out_shape=jax.ShapeDtypeStruct((4, 64, 2048), jnp.bfloat16),
        in_specs=[SMEM] + [VMEM] * 4,
        out_specs=VMEM,
        scratch_shapes=[pltpu.VMEM(WHOLE, jnp.bfloat16)],
        compiler_params=pltpu.CompilerParams(vmem_limit_bytes=16 * 1024 * 1024),
    )(ids, *most, block)


def body(tokens, norm_gain, w_gate, w_up, w_down, post_gain):
    own = jnp.concatenate([w_gate, w_up, w_down.T], axis=0)
    own = jnp.broadcast_to(own[None], (8, *own.shape))
    block = lax.all_to_all(own, PLANE, 0, 0, tiled=True, axis_index_groups=first_groups())
    own_normed = rms_scale(tokens.astype(jnp.float32), norm_gain).astype(jnp.bfloat16)
    copies = jnp.broadcast_to(own_normed[None], (8, *own_normed.shape))
    blocks = [block]
    even = odd = block
    for _ in range(3):
        new_even = exchange(odd, 0)
        odd = exchange(even, 1)
        even = new_even
        blocks += [even, odd]
    final = exchange(odd, 0)
    normed = lax.all_to_all(copies, ("x", "c"), 0, 0, tiled=True)
    core = lax.axis_index("c")
    base = jnp.where(core == 0, lax.axis_index("zl"), lax.axis_index("y"))
    ids = jnp.stack([base, core, 1 - core]).astype(jnp.int32)
    most = most_of(ids, normed, blocks)
    send = partial_of(ids, most, final)
    other = lax.ppermute(send, "c", [(0, 1), (1, 0)])
    ids = jnp.stack([base, core, core]).astype(jnp.int32)
    keep = partial_of(ids, most, final)
    pair = (keep.astype(jnp.float32) + other.astype(jnp.float32)).astype(jnp.bfloat16)
    arrived = lax.all_to_all(pair, "x", split_axis=0, concat_axis=0, tiled=True)
    summed = arrived.astype(jnp.float32).sum(axis=0)
    return rms_scale(summed, post_gain).astype(jnp.bfloat16)


def solution(mesh):
    finer = Mesh(mesh.devices.reshape(2, 8, 8, 4, 2), ALL)
    split = P(("zl", "y"), ("x", "c"))
    return jax.shard_map(
        body,
        mesh=finer,
        in_specs=(P(ALL, None), P(), split, split, P(("x", "c"), ("zl", "y")), P()),
        out_specs=P(ALL, None),
        check_vma=False,
    )
```

```python
import jax
import jax.numpy as jnp
from jax import lax
from jax.experimental import pallas as pl
from jax.experimental.pallas import tpu as pltpu
from jax.sharding import Mesh
from jax.sharding import PartitionSpec as P


EPS = 1e-06
ALL = ("zh", "zl", "y", "x", "c")
PLANE = ("zh", "zl", "y", "c")


def rms_scale(values, gain):
    return values * lax.rsqrt(jnp.mean(values * values, axis=-1, keepdims=True) + EPS) * gain


def first_groups():
    at = lambda zh, zl, y, c: ((zh * 8 + zl) * 8 + y) * 2 + c
    groups = [[at(zh, zl, y, 0) for y in range(8)] for zh in range(2) for zl in range(8)]
    return groups + [[at(zh, zl, y, 1) for zl in range(8)] for zh in range(2) for y in range(8)]


def partner(i, kind):
    return ((i + kind) ^ 1) - kind


def exchange(x, kind):
    pairs = []
    for z in range(16):
        for y in range(8):
            here = (z * 8 + y) * 2
            pairs.append((here, (partner(z, kind) % 16 * 8 + y) * 2))
            pairs.append((here + 1, (z * 8 + partner(y, kind) % 8) * 2 + 1))
    return lax.ppermute(x, PLANE, pairs)


def most_kernel(ids, normed, *refs):
    blocks = refs[0:7]
    gate_up, x_last, down, gate_w, up_w = refs[7:12]
    base, core = ids[0], ids[1]
    side = 1 - 2 * (base & 1)
    weights = (gate_w, up_w, down)
    classes = [(base + 8 + n * side) & 7 for n in (0, 1, -1, 2, -2, 3, -3)]
    last = (base + 4) & 7
    empty = jnp.zeros((8, 32, 384), jnp.bfloat16)

    @pl.when(core == 0)
    def _():
        for n, w in enumerate(weights):
            w[last] = empty
            for blk, at in zip(blocks, classes):
                w[at] = blk[:, 32 * n : 32 * n + 32, :]

    @pl.when(core == 1)
    def _():
        for n, w in enumerate(weights):
            w[:, last] = empty
            for blk, at in zip(blocks, classes):
                w[:, at] = blk[:, 32 * n : 32 * n + 32, :]

    x = normed[...].reshape(512, 2048)
    for n, w in enumerate((gate_w, up_w)):
        acc = jnp.dot(x, w[...].reshape(2048, 384), preferred_element_type=jnp.float32)
        gate_up[n] = acc.reshape(4, 2, 64, 384)
    row = lax.broadcasted_iota(jnp.int32, (2048, 256), 0)
    j = lax.broadcasted_iota(jnp.int32, (2048, 256), 1)
    wanted = jnp.where(core == 0, last * 256 + j, (j >> 5) * 256 + last * 32 + (j & 31))
    pick = jnp.where(row == wanted, 1.0, 0.0).astype(jnp.bfloat16)
    picked = jnp.dot(x, pick, preferred_element_type=jnp.float32)
    x_last[...] = picked.astype(jnp.bfloat16).reshape(4, 2, 64, 256)


def last_kernel(ids, gate_up, x_last, most_down, blk, out, down):
    base, core, which = ids[0], ids[1], ids[2]
    last = (base + 4) & 7
    down[...] = most_down[...]

    @pl.when(core == 0)
    def _():
        down[last] = blk[:, 64:96, :]

    @pl.when(core == 1)
    def _():
        down[:, last] = blk[:, 64:96, :]

    x = x_last[:, which].reshape(256, 256)
    sums = []
    for n in range(2):
        w = blk[:, 32 * n : 32 * n + 32, :].reshape(256, 384)
        rest = jnp.dot(x, w, preferred_element_type=jnp.float32)
        sums.append(gate_up[n, :, which].reshape(256, 384) + rest)
    gate, up = sums
    hidden = (gate / (1.0 + jnp.exp(-gate)) * up).astype(jnp.bfloat16)
    nt = (((1,), (1,)), ((), ()))
    part = lax.dot_general(hidden, down[...].reshape(2048, 384), nt, preferred_element_type=jnp.float32)
    part = part.astype(jnp.bfloat16)
    for k in range(4):
        out[ids[3] ^ k] = part[64 * k : 64 * k + 64]


VMEM = pl.BlockSpec(memory_space=pltpu.VMEM)
SMEM = pl.BlockSpec(memory_space=pltpu.SMEM)
WHOLE = (8, 8, 32, 384)


def most_of(ids, normed, blocks):
    return pl.pallas_call(
        most_kernel,
        out_shape=(
            jax.ShapeDtypeStruct((2, 4, 2, 64, 384), jnp.float32),
            jax.ShapeDtypeStruct((4, 2, 64, 256), jnp.bfloat16),
            jax.ShapeDtypeStruct(WHOLE, jnp.bfloat16),
        ),
        in_specs=[SMEM] + [VMEM] * 8,
        out_specs=(VMEM, VMEM, VMEM),
        scratch_shapes=[pltpu.VMEM(WHOLE, jnp.bfloat16)] * 2,
        compiler_params=pltpu.CompilerParams(vmem_limit_bytes=46 * 1024 * 1024),
        name="most",
    )(ids, normed, *blocks)


def partial_of(ids, most, block):
    return pl.pallas_call(
        last_kernel,
        out_shape=jax.ShapeDtypeStruct((4, 64, 2048), jnp.bfloat16),
        in_specs=[SMEM] + [VMEM] * 4,
        out_specs=VMEM,
        scratch_shapes=[pltpu.VMEM(WHOLE, jnp.bfloat16)],
        compiler_params=pltpu.CompilerParams(vmem_limit_bytes=16 * 1024 * 1024),
    )(ids, *most, block)


def body(tokens, norm_gain, w_gate, w_up, w_down, post_gain):
    own = jnp.concatenate([w_gate, w_up, w_down.T], axis=0)
    own = jnp.broadcast_to(own[None], (8, *own.shape))
    block = lax.all_to_all(own, PLANE, 0, 0, tiled=True, axis_index_groups=first_groups())
    own_normed = rms_scale(tokens.astype(jnp.float32), norm_gain).astype(jnp.bfloat16)
    copies = jnp.broadcast_to(own_normed[None], (8, *own_normed.shape))
    blocks = [block]
    even = odd = block
    for _ in range(3):
        new_even = exchange(odd, 0)
        odd = exchange(even, 1)
        even = new_even
        blocks += [even, odd]
    final = exchange(odd, 0)
    normed = lax.all_to_all(copies, ("x", "c"), 0, 0, tiled=True)
    core, col = lax.axis_index("c"), lax.axis_index("x")
    base = jnp.where(core == 0, lax.axis_index("zl"), lax.axis_index("y"))
    ids = jnp.stack([base, core, 1 - core, col]).astype(jnp.int32)
    most = most_of(ids, normed, blocks)
    send = partial_of(ids, most, final)
    other = lax.ppermute(send, "c", [(0, 1), (1, 0)])
    ids = jnp.stack([base, core, core, col]).astype(jnp.int32)
    keep = partial_of(ids, most, final)
    pair = [keep[k].astype(jnp.float32) + other[k].astype(jnp.float32) for k in range(4)]
    summed = pair[0]
    for k in (2, 1, 3):
        got = lax.ppermute(pair[k].astype(jnp.bfloat16), "x", [(x, x ^ k) for x in range(4)])
        summed = summed + got.astype(jnp.float32)
    return rms_scale(summed, post_gain).astype(jnp.bfloat16)


def solution(mesh):
    finer = Mesh(mesh.devices.reshape(2, 8, 8, 4, 2), ALL)
    split = P(("zl", "y"), ("x", "c"))
    return jax.shard_map(
        body,
        mesh=finer,
        in_specs=(P(ALL, None), P(), split, split, P(("x", "c"), ("zl", "y")), P()),
        out_specs=P(ALL, None),
        check_vma=False,
    )
```

```python
import jax
import jax.numpy as jnp
from jax import lax
from jax.experimental import pallas as pl
from jax.experimental.pallas import tpu as pltpu
from jax.sharding import Mesh
from jax.sharding import PartitionSpec as P


EPS = 1e-06
ALL = ("zh", "zl", "y", "x", "c")
PLANE = ("zh", "zl", "y", "c")


def rms_scale(values, gain):
    return values * lax.rsqrt(jnp.mean(values * values, axis=-1, keepdims=True) + EPS) * gain


def first_groups():
    at = lambda zh, zl, y, c: ((zh * 8 + zl) * 8 + y) * 2 + c
    groups = [[at(zh, zl, y, 0) for y in range(8)] for zh in range(2) for zl in range(8)]
    return groups + [[at(zh, zl, y, 1) for zl in range(8)] for zh in range(2) for y in range(8)]


def partner(i, kind):
    return ((i + kind) ^ 1) - kind


def exchange(x, kind):
    pairs = []
    for z in range(16):
        for y in range(8):
            here = (z * 8 + y) * 2
            pairs.append((here, (partner(z, kind) % 16 * 8 + y) * 2))
            pairs.append((here + 1, (z * 8 + partner(y, kind) % 8) * 2 + 1))
    return lax.ppermute(x, PLANE, pairs)


def copies_kernel(w_gate, w_up, w_down, out):
    for k in range(8):
        out[k, 0:32] = w_gate[...]
        out[k, 32:64] = w_up[...]
        out[k, 64:96] = w_down[...]


def most_kernel(ids, normed, *refs):
    blocks = refs[0:7]
    gate_up, x_last, down, gate_w, up_w = refs[7:12]
    base, core = ids[0], ids[1]
    side = 1 - 2 * (base & 1)
    weights = (gate_w, up_w, down)
    classes = [(base + 8 + n * side) & 7 for n in (0, 1, -1, 2, -2, 3, -3)]
    last = (base + 4) & 7
    empty = jnp.zeros((8, 32, 384), jnp.bfloat16)

    @pl.when(core == 0)
    def _():
        for n, w in enumerate(weights):
            w[last] = empty
            for blk, at in zip(blocks, classes):
                w[at] = blk[:, 32 * n : 32 * n + 32, :]

    @pl.when(core == 1)
    def _():
        for n, w in enumerate(weights):
            w[:, last] = empty
            for blk, at in zip(blocks, classes):
                w[:, at] = blk[:, 32 * n : 32 * n + 32, :]

    x = normed[...].reshape(512, 2048)
    for n, w in enumerate((gate_w, up_w)):
        acc = jnp.dot(x, w[...].reshape(2048, 384), preferred_element_type=jnp.float32)
        gate_up[n] = acc.reshape(4, 2, 64, 384)
    row = lax.broadcasted_iota(jnp.int32, (2048, 256), 0)
    j = lax.broadcasted_iota(jnp.int32, (2048, 256), 1)
    wanted = jnp.where(core == 0, last * 256 + j, (j >> 5) * 256 + last * 32 + (j & 31))
    pick = jnp.where(row == wanted, 1.0, 0.0).astype(jnp.bfloat16)
    picked = jnp.dot(x, pick, preferred_element_type=jnp.float32)
    x_last[...] = picked.astype(jnp.bfloat16).reshape(4, 2, 64, 256)


def last_kernel(ids, gate_up, x_last, most_down, blk, out, down):
    base, core, which = ids[0], ids[1], ids[2]
    last = (base + 4) & 7
    down[...] = most_down[...]

    @pl.when(core == 0)
    def _():
        down[last] = blk[:, 64:96, :]

    @pl.when(core == 1)
    def _():
        down[:, last] = blk[:, 64:96, :]

    x = x_last[:, which].reshape(256, 256)
    sums = []
    for n in range(2):
        w = blk[:, 32 * n : 32 * n + 32, :].reshape(256, 384)
        rest = jnp.dot(x, w, preferred_element_type=jnp.float32)
        sums.append(gate_up[n, :, which].reshape(256, 384) + rest)
    gate, up = sums
    hidden = (gate / (1.0 + jnp.exp(-gate)) * up).astype(jnp.bfloat16)
    nt = (((1,), (1,)), ((), ()))
    part = lax.dot_general(hidden, down[...].reshape(2048, 384), nt, preferred_element_type=jnp.float32)
    part = part.astype(jnp.bfloat16)
    for k in range(4):
        out[ids[3] ^ k] = part[64 * k : 64 * k + 64]


VMEM = pl.BlockSpec(memory_space=pltpu.VMEM)
SMEM = pl.BlockSpec(memory_space=pltpu.SMEM)
WHOLE = (8, 8, 32, 384)


def most_of(ids, normed, blocks):
    return pl.pallas_call(
        most_kernel,
        out_shape=(
            jax.ShapeDtypeStruct((2, 4, 2, 64, 384), jnp.float32),
            jax.ShapeDtypeStruct((4, 2, 64, 256), jnp.bfloat16),
            jax.ShapeDtypeStruct(WHOLE, jnp.bfloat16),
        ),
        in_specs=[SMEM] + [VMEM] * 8,
        out_specs=(VMEM, VMEM, VMEM),
        scratch_shapes=[pltpu.VMEM(WHOLE, jnp.bfloat16)] * 2,
        compiler_params=pltpu.CompilerParams(vmem_limit_bytes=46 * 1024 * 1024),
        name="most",
    )(ids, normed, *blocks)


def partial_of(ids, most, block):
    return pl.pallas_call(
        last_kernel,
        out_shape=jax.ShapeDtypeStruct((4, 64, 2048), jnp.bfloat16),
        in_specs=[SMEM] + [VMEM] * 4,
        out_specs=VMEM,
        scratch_shapes=[pltpu.VMEM(WHOLE, jnp.bfloat16)],
        compiler_params=pltpu.CompilerParams(vmem_limit_bytes=16 * 1024 * 1024),
    )(ids, *most, block)


def body(tokens, norm_gain, w_gate, w_up, w_down, post_gain):
    own = pl.pallas_call(
        copies_kernel,
        out_shape=jax.ShapeDtypeStruct((8, 96, 384), jnp.bfloat16),
        in_specs=[VMEM] * 3,
        out_specs=VMEM,
        name="copies",
    )(w_gate, w_up, w_down.T)
    block = lax.all_to_all(own, PLANE, 0, 0, tiled=True, axis_index_groups=first_groups())
    own_normed = rms_scale(tokens.astype(jnp.float32), norm_gain).astype(jnp.bfloat16)
    copies = jnp.broadcast_to(own_normed[None], (8, *own_normed.shape))
    blocks = [block]
    even = odd = block
    for _ in range(3):
        new_even = exchange(odd, 0)
        odd = exchange(even, 1)
        even = new_even
        blocks += [even, odd]
    final = exchange(odd, 0)
    normed = lax.all_to_all(copies, ("x", "c"), 0, 0, tiled=True)
    core, col = lax.axis_index("c"), lax.axis_index("x")
    base = jnp.where(core == 0, lax.axis_index("zl"), lax.axis_index("y"))
    ids = jnp.stack([base, core, 1 - core, col]).astype(jnp.int32)
    most = most_of(ids, normed, blocks)
    send = partial_of(ids, most, final)
    other = lax.ppermute(send, "c", [(0, 1), (1, 0)])
    ids = jnp.stack([base, core, core, col]).astype(jnp.int32)
    keep = partial_of(ids, most, final)
    pair = [keep[k].astype(jnp.float32) + other[k].astype(jnp.float32) for k in range(4)]
    summed = pair[0]
    for k in (2, 1, 3):
        got = lax.ppermute(pair[k].astype(jnp.bfloat16), "x", [(x, x ^ k) for x in range(4)])
        summed = summed + got.astype(jnp.float32)
    return rms_scale(summed, post_gain).astype(jnp.bfloat16)


def solution(mesh):
    finer = Mesh(mesh.devices.reshape(2, 8, 8, 4, 2), ALL)
    split = P(("zl", "y"), ("x", "c"))
    return jax.shard_map(
        body,
        mesh=finer,
        in_specs=(P(ALL, None), P(), split, split, P(("x", "c"), ("zl", "y")), P()),
        out_specs=P(ALL, None),
        check_vma=False,
    )
```

```python
import jax
import jax.numpy as jnp
from jax import lax
from jax.experimental import pallas as pl
from jax.experimental.pallas import tpu as pltpu
from jax.sharding import Mesh
from jax.sharding import PartitionSpec as P


EPS = 1e-06
ALL = ("zh", "zl", "y", "x", "c")
PLANE = ("zh", "zl", "y", "c")


def rms_scale(values, gain):
    return values * lax.rsqrt(jnp.mean(values * values, axis=-1, keepdims=True) + EPS) * gain


def first_groups():
    at = lambda zh, zl, y, c: ((zh * 8 + zl) * 8 + y) * 2 + c
    groups = [[at(zh, zl, y, 0) for y in range(8)] for zh in range(2) for zl in range(8)]
    return groups + [[at(zh, zl, y, 1) for zl in range(8)] for zh in range(2) for y in range(8)]


def partner(i, kind):
    return ((i + kind) ^ 1) - kind


def exchange(x, kind):
    pairs = []
    for z in range(16):
        for y in range(8):
            here = (z * 8 + y) * 2
            pairs.append((here, (partner(z, kind) % 16 * 8 + y) * 2))
            pairs.append((here + 1, (z * 8 + partner(y, kind) % 8) * 2 + 1))
    return lax.ppermute(x, PLANE, pairs)


def most_kernel(ids, normed, *refs):
    blocks = refs[0:7]
    gate_up, x_last, down, gate_w, up_w = refs[7:12]
    base, core = ids[0], ids[1]
    side = 1 - 2 * (base & 1)
    weights = (gate_w, up_w, down)
    classes = [(base + 8 + n * side) & 7 for n in (0, 1, -1, 2, -2, 3, -3)]
    last = (base + 4) & 7
    empty = jnp.zeros((8, 32, 384), jnp.bfloat16)

    @pl.when(core == 0)
    def _():
        for n, w in enumerate(weights):
            w[last] = empty
            for blk, at in zip(blocks, classes):
                w[at] = blk[:, 32 * n : 32 * n + 32, :]

    @pl.when(core == 1)
    def _():
        for n, w in enumerate(weights):
            w[:, last] = empty
            for blk, at in zip(blocks, classes):
                w[:, at] = blk[:, 32 * n : 32 * n + 32, :]

    x = normed[...].reshape(512, 2048)
    for n, w in enumerate((gate_w, up_w)):
        acc = jnp.dot(x, w[...].reshape(2048, 384), preferred_element_type=jnp.float32)
        gate_up[n] = acc.reshape(4, 2, 64, 384)
    row = lax.broadcasted_iota(jnp.int32, (2048, 256), 0)
    j = lax.broadcasted_iota(jnp.int32, (2048, 256), 1)
    wanted = jnp.where(core == 0, last * 256 + j, (j >> 5) * 256 + last * 32 + (j & 31))
    pick = jnp.where(row == wanted, 1.0, 0.0).astype(jnp.bfloat16)
    picked = jnp.dot(x, pick, preferred_element_type=jnp.float32)
    x_last[...] = picked.astype(jnp.bfloat16).reshape(4, 2, 64, 256)


def last_kernel(ids, gate_up, x_last, most_down, blk, out, out_own, down):
    base, core, which = ids[0], ids[1], ids[2]
    last = (base + 4) & 7
    down[...] = most_down[...]

    @pl.when(core == 0)
    def _():
        down[last] = blk[:, 64:96, :]

    @pl.when(core == 1)
    def _():
        down[:, last] = blk[:, 64:96, :]

    x = x_last[:, which].reshape(256, 256)
    sums = []
    for n in range(2):
        w = blk[:, 32 * n : 32 * n + 32, :].reshape(256, 384)
        rest = jnp.dot(x, w, preferred_element_type=jnp.float32)
        sums.append(gate_up[n, :, which].reshape(256, 384) + rest)
    gate, up = sums
    hidden = (gate / (1.0 + jnp.exp(-gate)) * up).astype(jnp.bfloat16)
    nt = (((1,), (1,)), ((), ()))
    part = lax.dot_general(hidden, down[...].reshape(2048, 384), nt, preferred_element_type=jnp.float32)
    part = part.astype(jnp.bfloat16)
    for k in range(4):
        to = ids[3] ^ k

        @pl.when(to == 0)
        def _():
            out_own[...] = part[64 * k : 64 * k + 64]

        @pl.when(to != 0)
        def _():
            out[to - 1] = part[64 * k : 64 * k + 64]


VMEM = pl.BlockSpec(memory_space=pltpu.VMEM)
SMEM = pl.BlockSpec(memory_space=pltpu.SMEM)
WHOLE = (8, 8, 32, 384)


def most_of(ids, normed, blocks):
    return pl.pallas_call(
        most_kernel,
        out_shape=(
            jax.ShapeDtypeStruct((2, 4, 2, 64, 384), jnp.float32),
            jax.ShapeDtypeStruct((4, 2, 64, 256), jnp.bfloat16),
            jax.ShapeDtypeStruct(WHOLE, jnp.bfloat16),
        ),
        in_specs=[SMEM] + [VMEM] * 8,
        out_specs=(VMEM, VMEM, VMEM),
        scratch_shapes=[pltpu.VMEM(WHOLE, jnp.bfloat16)] * 2,
        compiler_params=pltpu.CompilerParams(vmem_limit_bytes=46 * 1024 * 1024),
        name="most",
    )(ids, normed, *blocks)


def partial_of(ids, most, block):
    return pl.pallas_call(
        last_kernel,
        out_shape=(jax.ShapeDtypeStruct((3, 64, 2048), jnp.bfloat16), jax.ShapeDtypeStruct((64, 2048), jnp.bfloat16)),
        in_specs=[SMEM] + [VMEM] * 4,
        out_specs=(VMEM, VMEM),
        scratch_shapes=[pltpu.VMEM(WHOLE, jnp.bfloat16)],
        compiler_params=pltpu.CompilerParams(vmem_limit_bytes=16 * 1024 * 1024),
    )(ids, *most, block)


def body(tokens, norm_gain, w_gate, w_up, w_down, post_gain):
    own = jnp.concatenate([w_gate, w_up, w_down.T], axis=0)
    own = jnp.broadcast_to(own[None], (8, *own.shape))
    block = lax.all_to_all(own, PLANE, 0, 0, tiled=True, axis_index_groups=first_groups())
    own_normed = rms_scale(tokens.astype(jnp.float32), norm_gain).astype(jnp.bfloat16)
    copies = jnp.broadcast_to(own_normed[None], (8, *own_normed.shape))
    blocks = [block]
    even = odd = block
    for _ in range(3):
        new_even = exchange(odd, 0)
        odd = exchange(even, 1)
        even = new_even
        blocks += [even, odd]
    final = exchange(odd, 0)
    normed = lax.all_to_all(copies, ("x", "c"), 0, 0, tiled=True)
    core, col = lax.axis_index("c"), lax.axis_index("x")
    base = jnp.where(core == 0, lax.axis_index("zl"), lax.axis_index("y"))
    ids = jnp.stack([base, core, 1 - core, col]).astype(jnp.int32)
    most = most_of(ids, normed, blocks)
    send, send_own = partial_of(ids, most, final)
    other = lax.ppermute(send, "c", [(0, 1), (1, 0)])
    other_own = lax.ppermute(send_own, "c", [(0, 1), (1, 0)])
    ids = jnp.stack([base, core, core, col]).astype(jnp.int32)
    keep, keep_own = partial_of(ids, most, final)
    pair = [keep[k].astype(jnp.float32) + other[k].astype(jnp.float32) for k in range(3)]
    summed = keep_own.astype(jnp.float32) + other_own.astype(jnp.float32)
    for k in (2, 1, 3):
        got = lax.ppermute(pair[k - 1].astype(jnp.bfloat16), "x", [(x, x ^ k) for x in range(4)])
        summed = summed + got.astype(jnp.float32)
    return rms_scale(summed, post_gain).astype(jnp.bfloat16)


def solution(mesh):
    finer = Mesh(mesh.devices.reshape(2, 8, 8, 4, 2), ALL)
    split = P(("zl", "y"), ("x", "c"))
    return jax.shard_map(
        body,
        mesh=finer,
        in_specs=(P(ALL, None), P(), split, split, P(("x", "c"), ("zl", "y")), P()),
        out_specs=P(ALL, None),
        check_vma=False,
    )
```
